32 devices in a mesh: sp: 4 (over z), tp: 4 (over y, x), dp: 2 (over core).
Axes of the slice: x: 2, y: 2, z: 4, core: 2. Of those that a mesh axis runs over, the one named last changes fastest.
Arguments:
- latent_in: bfloat16 [3072, 2048], P(('dp', 'sp', 'tp')), parts along dimension 0, may hold values from -6 to 6
- condition: bfloat16 [4096], P(('dp', 'sp')), parts along dimension 0, may hold values from -8 to 8
- context_latent: bfloat16 [1024, 256], P(('dp', 'sp')), parts along dimension 0, may hold values from -6 to 6
- context_rope: bfloat16 [1024, 64], P(('dp', 'sp')), parts along dimension 0, may hold values from -6 to 6
- shift_weight: bfloat16 [2048, 2048], P('sp', 'tp'), may hold values from -0.125 to 0.125
- scale_weight: bfloat16 [2048, 2048], P('sp', 'tp'), may hold values from -0.125 to 0.125
- gate_weight: bfloat16 [2048, 2048], P('sp', 'tp'), may hold values from -0.125 to 0.125
- norm_gain: float32 [2048], replicated, may hold values from 0.1 to 1.9
- down_query: bfloat16 [2048, 512], replicated, may hold values from -0.125 to 0.125
- down_latent: bfloat16 [2048, 256], replicated, may hold values from -0.125 to 0.125
- down_rope: bfloat16 [2048, 64], replicated, may hold values from -0.125 to 0.125
- query_gain: float32 [512], replicated, may hold values from 0.5 to 60
- latent_gain: float32 [256], replicated, may hold values from 0.1 to 1.9
- up_query: bfloat16 [512, 1536], P(None, 'tp'), may hold values from -0.25 to 0.25
- up_key: bfloat16 [256, 1024], P(None, 'tp'), may hold values from -0.375 to 0.375
- up_value: bfloat16 [256, 1024], P(None, 'tp'), may hold values from -0.375 to 0.375
- context_bias: float32 [8], P('tp'), may hold values from 1 to 2.5
- out_weight: bfloat16 [1024, 2048], replicated, may hold values from -3 to 3
Outputs:
- mixed_out: bfloat16 [3072, 2048], P(('dp', 'sp', 'tp')), parts along dimension 0
The draws below stay inside these ranges and needn't reach their ends.
There are 2 independent parts, one for each index of `dp`. The reference program is written for one: setup_inputs(seed, part) draws one part's arguments, and reference() takes and returns one part's arrays. A program takes and returns all parts, laid end to end along the dimension named above; an argument that names none is the same for every part. Nothing has to cross between parts.
All inputs are finite; a program needn't handle non-finite values.
Results may differ from the reference program's by a relative error of at most 0.039.
The reference program's roundings to bfloat16 on the way count: a program that leaves them out, or rounds other values in their place, can miss the bound.
Values may be sent and summed in bfloat16 or wider, within the bound.
A program may use at most 128 MiB of HBM per device.

```python
import math
import jax
import jax.numpy as jnp
from jax import lax

D = 2048
HEADS = 8
QK_NOPE = 128
QK_ROPE = 64
V_HEAD = 128
Q_RANK = 512
KV_RANK = 256
GRID_W = 64
CTX = 512
TOKENS = 1536


def draw_query_gain(key, part):
    gains = jax.random.uniform(key, (Q_RANK,), jnp.float32, 0.5, 1.5)
    return gains


def levels(rng, shape, cuts, low, high):
    def one(axis_at, blocks):
        draws = jax.random.uniform(jax.random.fold_in(jax.random.fold_in(rng, 6), axis_at), (blocks,), jnp.float32, low / len(cuts), high / len(cuts))
        return jnp.repeat(jnp.exp(draws), shape[axis_at] // blocks).reshape((-1,) + (1,) * (len(shape) - axis_at - 1))

    gain = one(*cuts[0])
    for cut in cuts[1:]:
        gain = gain * one(*cut)
    return gain


def noise(own_key, extent, scale, reach, cuts=(), kind=jnp.bfloat16):
    level = levels(own_key, extent, cuts, -0.22, 0.18) if cuts else 1.0
    entries = jax.random.normal(own_key, extent, jnp.float32) * scale * level
    return jnp.minimum(jnp.maximum(entries, -reach), reach).astype(kind)


def setup_inputs(seed: int = 0, part: int = 0) -> dict:
    splits = jax.random.split(jax.random.key(seed), 19)
    part_splits = jax.random.split(jax.random.fold_in(splits[18], part), 19)
    latent_in = noise(part_splits[0], (TOKENS, D), 1.0, 6.0, ((0, 16),))
    condition = noise(part_splits[1], (D,), 2.0, 8.0, ((0, 4),))
    context_latent = noise(part_splits[2], (CTX, KV_RANK), 1.0, 6.0, ((0, 4),))
    context_rope = noise(part_splits[3], (CTX, QK_ROPE), 1.0, 6.0, ((0, 4),))
    shift_weight = noise(splits[4], (D, D), D ** -0.5, 0.125, ((0, 4), (1, 4)))
    scale_weight = noise(splits[5], (D, D), D ** -0.5, 0.125, ((0, 4), (1, 4)))
    gate_weight = noise(splits[6], (D, D), D ** -0.5, 0.125, ((0, 4), (1, 4)))
    norm_gain = jnp.clip(1.0 + 0.18 * jax.random.normal(splits[7], (D,), jnp.float32), 0.1, 1.9)
    down_query = noise(splits[8], (D, Q_RANK), D ** -0.5, 0.125)
    down_latent = noise(splits[9], (D, KV_RANK), D ** -0.5, 0.125)
    down_rope = noise(splits[10], (D, QK_ROPE), D ** -0.5, 0.125)
    query_gain = draw_query_gain(jax.random.fold_in(splits[18], 71), part)
    latent_gain = jnp.clip(1.0 + 0.18 * jax.random.normal(splits[12], (KV_RANK,), jnp.float32), 0.1, 1.9)
    up_query = noise(splits[13], (Q_RANK, HEADS * (QK_NOPE + QK_ROPE)), Q_RANK ** -0.5, 0.25, ((1, 4),))
    up_key = noise(splits[14], (KV_RANK, HEADS * QK_NOPE), KV_RANK ** -0.5, 0.375, ((1, 4),))
    up_value = noise(splits[15], (KV_RANK, HEADS * V_HEAD), KV_RANK ** -0.5, 0.375, ((1, 4),))
    context_bias = jnp.clip(1.0 + 1.5 * jax.random.uniform(splits[16], (HEADS,), jnp.float32) ** levels(splits[16], (HEADS,), ((0, 4),), -0.2, 0.2), 1.0, 2.5)
    out_weight = noise(splits[17], (HEADS * V_HEAD, D), 0.5, 3.0)
    return dict(latent_in=latent_in, condition=condition, context_latent=context_latent, context_rope=context_rope, shift_weight=shift_weight, scale_weight=scale_weight, gate_weight=gate_weight, norm_gain=norm_gain, down_query=down_query, down_latent=down_latent, down_rope=down_rope, query_gain=query_gain, latent_gain=latent_gain, up_query=up_query, up_key=up_key, up_value=up_value, context_bias=context_bias, out_weight=out_weight)


epsilon = 1e-06
rope_base = 10000.0

def rms_scaled(values, gain_vec):
    mean_sq = lax.optimization_barrier(jnp.mean(values * values, axis=-1, keepdims=True))
    return values * lax.rsqrt(mean_sq + epsilon) * gain_vec

def rope_tables(positions, rope_width):
    freq_count = rope_width // 4
    inverse = rope_base ** (-jnp.arange(freq_count, dtype=jnp.float32) / freq_count)
    grid_row = (positions // GRID_W).astype(jnp.float32)
    grid_col = (positions % GRID_W).astype(jnp.float32)
    row_angle = grid_row[:, None] * inverse
    col_angle = grid_col[:, None] * inverse
    angles = jnp.concatenate([row_angle, row_angle, col_angle, col_angle], axis=-1)
    return (jnp.cos(angles), jnp.sin(angles))

def rope_turn(values, cosine_table, sine_table):
    part_one, part_two, part_three, part_four = jnp.split(values, 4, axis=-1)
    turned = jnp.concatenate([-part_two, part_one, -part_four, part_three], axis=-1)
    return values * cosine_table + turned * sine_table

def reference(latent_in, condition, context_latent, context_rope, shift_weight, scale_weight, gate_weight, norm_gain, down_query, down_latent, down_rope, query_gain, latent_gain, up_query, up_key, up_value, context_bias, out_weight):
    activated = jax.nn.silu(condition.astype(jnp.float32)).astype(jnp.bfloat16)
    shift_vec = jnp.dot(activated, shift_weight, preferred_element_type=jnp.float32)
    scale_vec = jnp.dot(activated, scale_weight, preferred_element_type=jnp.float32)
    gate_vec = jnp.dot(activated, gate_weight, preferred_element_type=jnp.float32)
    residual_in = latent_in.astype(jnp.float32)
    normed = (rms_scaled(residual_in, norm_gain) * (1.0 + scale_vec) + shift_vec).astype(jnp.bfloat16)
    query_low = rms_scaled(jnp.dot(normed, down_query, preferred_element_type=jnp.float32), query_gain).astype(jnp.bfloat16)
    latent_low = rms_scaled(jnp.dot(normed, down_latent, preferred_element_type=jnp.float32), latent_gain).astype(jnp.bfloat16)
    positions = jnp.arange(TOKENS, dtype=jnp.int32)
    cosine_table, sine_table = rope_tables(positions, QK_ROPE)
    rope_keys = rope_turn(jnp.dot(normed, down_rope, preferred_element_type=jnp.float32), cosine_table, sine_table).astype(jnp.bfloat16)
    queries = jnp.dot(query_low, up_query, preferred_element_type=jnp.float32).reshape(TOKENS, HEADS, QK_NOPE + QK_ROPE)
    query_rope = rope_turn(queries[:, :, QK_NOPE:], cosine_table[:, None, :], sine_table[:, None, :])
    queries = jnp.concatenate([queries[:, :, :QK_NOPE], query_rope], axis=-1).astype(jnp.bfloat16)
    all_latent = jnp.concatenate([context_latent, latent_low], axis=0)
    all_rope = jnp.concatenate([context_rope, rope_keys], axis=0)
    key_count = CTX + TOKENS
    keys_nope = jnp.dot(all_latent, up_key, preferred_element_type=jnp.float32).astype(jnp.bfloat16).reshape(key_count, HEADS, QK_NOPE)
    values_all = jnp.dot(all_latent, up_value, preferred_element_type=jnp.float32).astype(jnp.bfloat16).reshape(key_count, HEADS, V_HEAD)
    bias_row = jnp.concatenate([jnp.broadcast_to(context_bias[:, None], (HEADS, CTX)), jnp.zeros((HEADS, TOKENS), jnp.float32)], axis=1)[:, None, :]
    keys_wide = keys_nope.astype(jnp.float32)
    rope_wide = all_rope.astype(jnp.float32)
    values_wide = values_all.astype(jnp.float32)
    block_rows = math.gcd(TOKENS, 512)
    query_blocks = queries.astype(jnp.float32).reshape(TOKENS // block_rows, block_rows, HEADS, QK_NOPE + QK_ROPE)
    score_scale = (QK_NOPE + QK_ROPE) ** (-0.5)

    def one_block(query_block):
        scores = jnp.einsum('thd,khd->htk', query_block[:, :, :QK_NOPE], keys_wide)
        scores = scores + jnp.einsum('thr,kr->htk', query_block[:, :, QK_NOPE:], rope_wide)
        scores = scores * score_scale + bias_row
        row_max = lax.optimization_barrier(jnp.max(scores, axis=-1, keepdims=True))
        weights = jnp.exp(scores - row_max)
        totals = lax.optimization_barrier(jnp.sum(weights, axis=-1))
        rounded = lax.optimization_barrier(weights.astype(jnp.bfloat16)).astype(jnp.float32)
        summed = jnp.einsum('htk,khd->htd', rounded, values_wide)
        return (summed / totals[:, :, None]).astype(jnp.bfloat16)
    outputs = lax.map(one_block, query_blocks)
    attended = outputs.transpose(0, 2, 1, 3).reshape(TOKENS, HEADS * V_HEAD)
    mixed = jnp.dot(attended, out_weight, preferred_element_type=jnp.float32)
    return (residual_in + gate_vec * mixed).astype(jnp.bfloat16)
```

```python
import functools
import math

import jax
import jax.numpy as jnp
from jax import lax
from jax.experimental import pallas as pl
from jax.experimental.pallas import tpu as pltpu
from jax.sharding import PartitionSpec as P

QK_NOPE = 128
QK_ROPE = 64
V_HEAD = 128
GRID_W = 64
EPS = 1e-06
ROPE_BASE = 10000.0
F32 = jnp.float32
BF16 = jnp.bfloat16
LOG2E = 1.4426950408889634


def dot(a, b):
    return jnp.dot(a, b, preferred_element_type=F32)


def dot_t(a, b):
    return lax.dot_general(a, b, (((1,), (1,)), ((), ())), preferred_element_type=F32)


def rms(values, gain):
    mean_sq = jnp.mean(values * values, axis=-1, keepdims=True)
    return values * lax.rsqrt(mean_sq + EPS) * gain


def turn(u, cos, sin_up, sin_down):
    width = u.shape[1]
    return u * cos + pltpu.roll(u, width - 16, 1) * sin_up + pltpu.roll(u, 16, 1) * sin_down


def kernel(sp, tp, *refs):
    (
        latent_hbm, cond_ref, ctx_lat_hbm, ctx_rope_hbm, shift_hbm, scale_hbm, gate_hbm,
        norm_gain_ref, dq_hbm, dl_hbm, dr_hbm, q_gain_ref, l_gain_ref, uq_hbm, uk_hbm, uv_hbm,
        bias_ref, ow_hbm, inv_ref,
        out_ref,
        x_ref, shift_w, scale_w, gate_w, dq, dl, dr, uq, uk, uv, ow, ctx_rope,
        base, cos_tab, sup_tab, sdn_tab, mod_z, mod_t, ctx_buf, lat_buf, q_buf, att_src, att_buf,
        mix, load_sem,
        mz_send, mz_recv, mt_send, mt_recv, cx_send, cx_recv, lz_send, lt_send, l_recv,
        q_send, q_recv, a_send, a_recv,
    ) = refs
    me_s = lax.axis_index("sp")
    me_t = lax.axis_index("tp")
    rows = x_ref.shape[0]
    group = rows * tp
    mcol = shift_w.shape[1]
    kv_rank = uk.shape[0]

    def zpeer(d):
        return lax.rem(me_s + d, sp)

    def tpeer(d):
        return lax.rem(me_t + d, tp)

    def remote(src, dst, ssem, rsem, axis, peer):
        return pltpu.make_async_remote_copy(
            src_ref=src, dst_ref=dst, send_sem=ssem, recv_sem=rsem,
            device_id={axis: peer}, device_id_type=pl.DeviceIdType.MESH,
        )

    loads = {}
    for i, (name, src, dst) in enumerate((
        ("shift", shift_hbm, shift_w), ("scale", scale_hbm, scale_w), ("gate", gate_hbm, gate_w),
        ("cl", ctx_lat_hbm, ctx_buf.at[me_s, :, pl.ds(0, kv_rank)]), ("cr", ctx_rope_hbm, ctx_rope),
        ("x", latent_hbm, x_ref), ("dl", dl_hbm, dl), ("dr", dr_hbm, dr), ("dq", dq_hbm, dq),
        ("uk", uk_hbm, uk), ("uv", uv_hbm, uv), ("uq", uq_hbm, uq), ("ow", ow_hbm, ow),
    )):
        loads[name] = pltpu.make_async_copy(src, dst, load_sem.at[i])
        loads[name].start()

    barrier = pltpu.get_barrier_semaphore()
    for d in range(1, sp):
        pl.semaphore_signal(barrier, inc=1, device_id={"sp": zpeer(d)}, device_id_type=pl.DeviceIdType.MESH)
    for d in range(1, tp):
        pl.semaphore_signal(barrier, inc=1, device_id={"tp": tpeer(d)}, device_id_type=pl.DeviceIdType.MESH)

    sends = []

    cond = cond_ref[...].astype(F32)
    act = (cond / (1.0 + jnp.exp(-cond))).astype(BF16)
    act = jnp.broadcast_to(act, (16, act.shape[1]))
    for i, (name, w) in enumerate((("shift", shift_w), ("scale", scale_w), ("gate", gate_w))):
        loads[name].wait()
        mod_z[me_s, i:i + 1, :] = dot(act, w[...])[0:1]
    mod_z[me_s, 3:4, :] = jnp.zeros((1, mcol), F32)
    pl.semaphore_wait(barrier, sp + tp - 2)
    for d in range(1, sp):
        c = remote(mod_z.at[me_s], mod_z.at[me_s], mz_send.at[d], mz_recv.at[me_s], "sp", zpeer(d))
        c.start()
        sends.append(c)
    loads["cl"].wait()
    loads["cr"].wait()
    cr = ctx_rope[...]
    ctx_buf[me_s, :, kv_rank:] = jnp.concatenate([cr, cr], axis=1)
    for d in range(1, sp):
        c = remote(ctx_buf.at[me_s], ctx_buf.at[me_s], cx_send.at[d], cx_recv.at[me_s], "sp", zpeer(d))
        c.start()
        sends.append(c)
    loads["x"].wait()
    base[...] = rms(x_ref[...].astype(F32), norm_gain_ref[...])

    for d in range(1, sp):
        s = zpeer(d)
        remote(mod_z.at[s], mod_z.at[s], mz_send.at[d], mz_recv.at[s], "sp", s).wait_recv()
    total = mod_z[0]
    for s in range(1, sp):
        total = total + mod_z[s]
    mod_t[me_t] = total
    for d in range(1, tp):
        c = remote(mod_t.at[me_t], mod_t.at[me_t], mt_send.at[d], mt_recv.at[me_t], "tp", tpeer(d))
        c.start()
        sends.append(c)

    pos = me_s * group + lax.broadcasted_iota(jnp.int32, (group, 128), 0)
    lane = lax.broadcasted_iota(jnp.int32, (group, 128), 1)
    coord = jnp.where(lax.rem(lane, 64) < 32, lax.div(pos, GRID_W), lax.rem(pos, GRID_W))
    angle = coord.astype(F32) * inv_ref[...]
    sin = jnp.sin(angle)
    first_run = lax.rem(lane, 32) < 16
    cos_tab[...] = jnp.cos(angle)
    sup_tab[...] = jnp.where(first_run, -sin, 0.0)
    sdn_tab[...] = jnp.where(first_run, 0.0, sin)

    loads["dl"].wait()
    loads["dr"].wait()
    normed = []
    low_l = low_r = None
    for d in range(tp):
        t = tpeer(d)
        if d:
            remote(mod_t.at[t], mod_t.at[t], mt_send.at[d], mt_recv.at[t], "tp", t).wait_recv()
        cols = pl.ds(pl.multiple_of(t * mcol, mcol), mcol)
        m = mod_t[t]
        nd = (base[:, cols] * (1.0 + m[1:2]) + m[0:1]).astype(BF16)
        normed.append((nd, cols))
        pl_, pr_ = dot(nd, dl[cols, :]), dot(nd, dr[cols, :])
        low_l = pl_ if low_l is None else low_l + pl_
        low_r = pr_ if low_r is None else low_r + pr_
    own = pl.ds(pl.multiple_of(me_t * rows, rows), rows)
    lat_buf[me_t, me_s, :, :kv_rank] = rms(low_l, l_gain_ref[...]).astype(BF16)
    lat_buf[me_t, me_s, :, kv_rank:] = turn(
        jnp.concatenate([low_r, low_r], axis=1), cos_tab[own, :], sup_tab[own, :], sdn_tab[own, :]
    ).astype(BF16)
    mine = lat_buf.at[me_t, me_s]
    for d in range(1, sp):
        c = remote(mine, mine, lz_send.at[d], l_recv.at[me_t, me_s], "sp", zpeer(d))
        c.start()
        sends.append(c)
    loads["dq"].wait()
    low_q = None
    for nd, cols in normed:
        pq = dot(nd, dq[cols, :])
        low_q = pq if low_q is None else low_q + pq
    q_buf[me_t] = rms(low_q, q_gain_ref[...]).astype(BF16)
    for d in range(1, tp):
        c = remote(q_buf.at[me_t], q_buf.at[me_t], q_send.at[d], q_recv.at[me_t], "tp", tpeer(d))
        c.start()
        sends.append(c)
    for d in range(1, tp):
        c = remote(mine, mine, lt_send.at[0, d], l_recv.at[me_t, me_s], "tp", tpeer(d))
        c.start()
        sends.append(c)

    def expand(block):
        low = block[:, :kv_rank]
        kn = dot(low, uk[...]).astype(BF16)
        v = dot(low, uv[...]).astype(BF16)
        kr = block[:, kv_rank:]
        return (
            jnp.concatenate([kn[:, :QK_NOPE], kr], axis=1),
            jnp.concatenate([kn[:, QK_NOPE:], kr], axis=1),
            v,
        )

    loads["uk"].wait()
    loads["uv"].wait()
    for d in range(1, sp):
        s = zpeer(d)
        remote(ctx_buf.at[s], ctx_buf.at[s], cx_send.at[d], cx_recv.at[s], "sp", s).wait_recv()
    ctx_kv = expand(ctx_buf[...].reshape(-1, ctx_buf.shape[2]))

    for d in range(1, sp):
        s = zpeer(d)
        slot = lat_buf.at[me_t, s]
        remote(slot, slot, lz_send.at[d], l_recv.at[me_t, s], "sp", s).wait_recv()
        for e in range(1, tp):
            c = remote(slot, slot, lt_send.at[d, e], l_recv.at[me_t, s], "tp", tpeer(e))
            c.start()
            sends.append(c)

    loads["uq"].wait()
    for d in range(1, tp):
        t = tpeer(d)
        remote(q_buf.at[t], q_buf.at[t], q_send.at[d], q_recv.at[t], "tp", t).wait_recv()
    q = dot(q_buf[...].reshape(group, q_buf.shape[2]), uq[...])
    one, two = q[:, 128:256], q[:, 256:384]
    low_half = lax.broadcasted_iota(jnp.int32, (group, 128), 1) < 64
    rope = turn(jnp.where(low_half, one, two), cos_tab[...], sup_tab[...], sdn_tab[...])
    nope = (q[:, :128], pltpu.roll(jnp.where(low_half, two, one), 64, 1))
    heads = (
        jnp.concatenate([nope[0], jnp.where(low_half, rope, 0.0)], axis=1).astype(BF16),
        jnp.concatenate([nope[1], jnp.where(low_half, 0.0, rope)], axis=1).astype(BF16),
    )
    factor = (QK_NOPE + QK_ROPE) ** (-0.5) * LOG2E

    def attend(state, kv, bias):
        result = []
        for h in range(2):
            s = dot_t(heads[h], kv[h]) * factor
            if bias:
                s = s + bias_ref[h] * LOG2E
            top = jnp.max(s, axis=-1, keepdims=True)
            v = kv[2][:, h * V_HEAD:(h + 1) * V_HEAD]
            if state is None:
                p = jnp.exp2(s - top)
                result.append((top, jnp.sum(p, axis=-1, keepdims=True), dot(p.astype(BF16), v)))
            else:
                m0, l0, a0 = state[h]
                top = jnp.maximum(top, m0)
                p = jnp.exp2(s - top)
                shrink = jnp.exp2(m0 - top)
                result.append((
                    top,
                    l0 * shrink + jnp.sum(p, axis=-1, keepdims=True),
                    a0 * shrink + dot(p.astype(BF16), v),
                ))
        return tuple(result)

    state = attend(None, ctx_kv, True)
    span = math.gcd(sp, 4)
    for d in range(tp):
        t = tpeer(d)
        if d:
            for e in range(sp):
                s = zpeer(e)
                slot = lat_buf.at[t, s]
                remote(slot, slot, lt_send.at[e, d], l_recv.at[t, s], "tp", t).wait_recv()

        def chunk(i, st, t=t):
            block = lat_buf[t, pl.ds(i * span, span)]
            return attend(st, expand(block.reshape(span * rows, block.shape[2])), False)

        if sp == span:
            state = chunk(0, state)
        else:
            state = lax.fori_loop(0, sp // span, chunk, state)
    for h in range(2):
        att = (state[h][2] / state[h][1]).astype(BF16)
        att_src[:, :, h * V_HEAD:(h + 1) * V_HEAD] = att.reshape(tp, rows, V_HEAD)
    for d in range(1, tp):
        t = tpeer(d)
        c = remote(att_src.at[t], att_buf.at[me_t], a_send.at[d], a_recv.at[me_t], "tp", t)
        c.start()
        sends.append(c)
    loads["ow"].wait()
    width = att_src.shape[2]
    for d in range(tp):
        t = tpeer(d)
        if d == 0:
            block = att_src[me_t]
        else:
            remote(att_buf.at[t], att_buf.at[t], a_send.at[d], a_recv.at[t], "tp", t).wait_recv()
            block = att_buf[t]
        part = dot(block, ow[pl.ds(pl.multiple_of(t * width, width), width), :])
        if d == 0:
            mix[...] = part
        else:
            mix[...] += part
    for t in range(tp):
        cols = slice(t * mcol, (t + 1) * mcol)
        out_ref[:, cols] = (x_ref[:, cols].astype(F32) + mod_t[t][2:3] * mix[:, cols]).astype(BF16)
    for c in sends:
        c.wait_send()


def solution(mesh):
    sp, tp = mesh.shape["sp"], mesh.shape["tp"]

    def on_device(
        latent_in, condition, context_latent, context_rope, shift_weight, scale_weight,
        gate_weight, norm_gain, down_query, down_latent, down_rope, query_gain, latent_gain,
        up_query, up_key, up_value, context_bias, out_weight,
    ):
        rows, width = latent_in.shape
        n = QK_ROPE // 4
        inverse = ROPE_BASE ** (-jnp.arange(n, dtype=F32) / n)
        inverse = jnp.tile(inverse, 128 // n)[None]
        group = rows * tp
        any_ = pl.BlockSpec(memory_space=pl.ANY)
        vmem = pl.BlockSpec(memory_space=pltpu.VMEM)
        smem = pl.BlockSpec(memory_space=pltpu.SMEM)
        kv_rank, q_rank = down_latent.shape[1], down_query.shape[1]
        heads = up_key.shape[1] // QK_NOPE
        block = kv_rank + 2 * QK_ROPE
        dma = pltpu.SemaphoreType.DMA

        def like(a):
            return pltpu.VMEM(a.shape, a.dtype)

        return pl.pallas_call(
            functools.partial(kernel, sp, tp),
            out_shape=jax.ShapeDtypeStruct(latent_in.shape, latent_in.dtype),
            in_specs=[any_, vmem, any_, any_, any_, any_, any_, vmem, any_, any_, any_, vmem, vmem,
                      any_, any_, any_, smem, any_, vmem],
            out_specs=vmem,
            scratch_shapes=[
                like(latent_in), like(shift_weight), like(scale_weight), like(gate_weight),
                like(down_query), like(down_latent), like(down_rope), like(up_query), like(up_key),
                like(up_value), like(out_weight), like(context_rope),
                pltpu.VMEM((rows, width), F32),
                pltpu.VMEM((group, 128), F32), pltpu.VMEM((group, 128), F32),
                pltpu.VMEM((group, 128), F32),
                pltpu.VMEM((sp, 4, shift_weight.shape[1]), F32),
                pltpu.VMEM((tp, 4, shift_weight.shape[1]), F32),
                pltpu.VMEM((sp, context_latent.shape[0], block), BF16),
                pltpu.VMEM((tp, sp, rows, block), BF16),
                pltpu.VMEM((tp, rows, q_rank), BF16),
                pltpu.VMEM((tp, rows, heads * V_HEAD), BF16),
                pltpu.VMEM((tp, rows, heads * V_HEAD), BF16),
                pltpu.VMEM((rows, width), F32),
                dma((13,)),
                dma((sp,)), dma((sp,)), dma((tp,)), dma((tp,)), dma((sp,)), dma((sp,)),
                dma((sp,)), dma((sp, tp)), dma((tp, sp)),
                dma((tp,)), dma((tp,)), dma((tp,)), dma((tp,)),
            ],
            compiler_params=pltpu.CompilerParams(
                collective_id=0, has_side_effects=True, vmem_limit_bytes=60 * 1024 * 1024
            ),
        )(
            latent_in, condition[None], context_latent, context_rope, shift_weight, scale_weight,
            gate_weight, norm_gain[None], down_query, down_latent, down_rope, query_gain[None],
            latent_gain[None], up_query, up_key, up_value, context_bias, out_weight, inverse,
        )

    in_specs = (
        P(("dp", "sp", "tp"), None), P(("dp", "sp")), P(("dp", "sp"), None), P(("dp", "sp"), None),
        P("sp", "tp"), P("sp", "tp"), P("sp", "tp"), P(), P(), P(), P(), P(), P(),
        P(None, "tp"), P(None, "tp"), P(None, "tp"), P("tp"), P(),
    )
    return jax.shard_map(
        on_device, mesh=mesh, in_specs=in_specs, out_specs=P(("dp", "sp", "tp"), None), check_vma=False
    )
```

```python
import functools
import math

import jax
import jax.numpy as jnp
import numpy as np
from jax import lax
from jax.experimental import pallas as pl
from jax.experimental.pallas import tpu as pltpu
from jax.sharding import PartitionSpec as P

QK_NOPE = 128
QK_ROPE = 64
V_HEAD = 128
GRID_W = 64
EPS = 1e-06
ROPE_BASE = 10000.0
F32 = jnp.float32
BF16 = jnp.bfloat16
LOG2E = 1.4426950408889634


def dot(a, b):
    return jnp.dot(a, b, preferred_element_type=F32)


def dot_t(a, b):
    return lax.dot_general(a, b, (((1,), (1,)), ((), ())), preferred_element_type=F32)


def rms(values, gain):
    mean_sq = jnp.mean(values * values, axis=-1, keepdims=True)
    return values * lax.rsqrt(mean_sq + EPS) * gain


def turn(u, cos, sin_up, sin_down):
    width = u.shape[1]
    return u * cos + pltpu.roll(u, width - 16, 1) * sin_up + pltpu.roll(u, 16, 1) * sin_down


def kernel(sp, tp, *refs):
    (
        latent_hbm, cond_ref, ctx_lat_hbm, ctx_rope_hbm, shift_hbm, scale_hbm, gate_hbm,
        norm_gain_ref, dq_hbm, dl_hbm, dr_hbm, q_gain_ref, l_gain_ref, uq_hbm, uk_hbm, uv_hbm,
        bias_ref, ow_hbm, inv_ref,
        out_ref,
        x_ref, shift_w, scale_w, gate_w, dq, dl, dr, uq, uk, uv, ow, ctx_rope,
        base, cos_tab, sup_tab, sdn_tab, mod_z, mod_t, ctx_buf, lat_buf, q_buf, att_src, att_buf,
        mix, load_sem,
        mz_send, mz_recv, mt_send, mt_recv, cx_send, cx_recv, lz_send, lz_recv, lt_send, l_recv,
        q_send, q_recv, a_send, a_recv,
    ) = refs
    me_s = lax.axis_index("sp")
    me_t = lax.axis_index("tp")
    rows = x_ref.shape[0]
    group = rows * tp
    mcol = shift_w.shape[1]
    kv_rank = uk.shape[0]

    def zpeer(d):
        return lax.rem(me_s + d, sp)

    def tpeer(d):
        return lax.rem(me_t + d, tp)

    def remote(src, dst, ssem, rsem, axis, peer):
        return pltpu.make_async_remote_copy(
            src_ref=src, dst_ref=dst, send_sem=ssem, recv_sem=rsem,
            device_id={axis: peer}, device_id_type=pl.DeviceIdType.MESH,
        )

    loads = {}
    for i, (name, src, dst) in enumerate((
        ("shift", shift_hbm, shift_w), ("scale", scale_hbm, scale_w), ("gate", gate_hbm, gate_w),
        ("cl", ctx_lat_hbm, ctx_buf.at[me_s, :, pl.ds(0, kv_rank)]), ("cr", ctx_rope_hbm, ctx_rope),
        ("x", latent_hbm, x_ref), ("dl", dl_hbm, dl), ("dr", dr_hbm, dr), ("dq", dq_hbm, dq),
        ("uk", uk_hbm, uk), ("uv", uv_hbm, uv), ("uq", uq_hbm, uq), ("ow", ow_hbm, ow),
    )):
        loads[name] = pltpu.make_async_copy(src, dst, load_sem.at[i])
    for name in ("shift", "scale", "gate", "cl", "cr", "x"):
        loads[name].start()

    barrier = pltpu.get_barrier_semaphore()
    for d in range(1, sp):
        pl.semaphore_signal(barrier, inc=1, device_id={"sp": zpeer(d)}, device_id_type=pl.DeviceIdType.MESH)
    for d in range(1, tp):
        pl.semaphore_signal(barrier, inc=1, device_id={"tp": tpeer(d)}, device_id_type=pl.DeviceIdType.MESH)

    sends = []

    cond = cond_ref[...].astype(F32)
    act = (cond / (1.0 + jnp.exp(-cond))).astype(BF16)
    act = jnp.broadcast_to(act, (16, act.shape[1]))
    for i, (name, w) in enumerate((("shift", shift_w), ("scale", scale_w), ("gate", gate_w))):
        loads[name].wait()
        mod_z[me_s, i:i + 1, :] = dot(act, w[...])[0:1]
    mod_z[me_s, 3:4, :] = jnp.zeros((1, mcol), F32)
    for name in ("dl", "dr", "dq", "uk", "uv", "uq", "ow"):
        loads[name].start()
    pl.semaphore_wait(barrier, sp + tp - 2)
    for d in range(1, sp):
        c = remote(mod_z.at[me_s], mod_z.at[me_s], mz_send.at[d], mz_recv.at[me_s], "sp", zpeer(d))
        c.start()
        sends.append(c)
    loads["cl"].wait()
    loads["cr"].wait()
    cr = ctx_rope[...].astype(F32)
    cr = jnp.concatenate([cr, cr], axis=0)
    ctx_buf[me_s, :, kv_rank:] = jnp.transpose(cr).astype(BF16)
    for d in range(1, sp):
        c = remote(ctx_buf.at[me_s], ctx_buf.at[me_s], cx_send.at[d], cx_recv.at[me_s], "sp", zpeer(d))
        c.start()
        sends.append(c)
    loads["x"].wait()
    base[...] = rms(x_ref[...].astype(F32), norm_gain_ref[...])

    for d in range(1, sp):
        s = zpeer(d)
        remote(mod_z.at[s], mod_z.at[s], mz_send.at[d], mz_recv.at[s], "sp", s).wait_recv()
    total = mod_z[0]
    for s in range(1, sp):
        total = total + mod_z[s]
    mod_t[me_t] = total
    for d in range(1, tp):
        c = remote(mod_t.at[me_t], mod_t.at[me_t], mt_send.at[d], mt_recv.at[me_t], "tp", tpeer(d))
        c.start()
        sends.append(c)

    pos = me_s * group + lax.broadcasted_iota(jnp.int32, (group, 128), 0)
    lane = lax.broadcasted_iota(jnp.int32, (group, 128), 1)
    coord = jnp.where(lax.rem(lane, 64) < 32, lax.div(pos, GRID_W), lax.rem(pos, GRID_W))
    angle = coord.astype(F32) * inv_ref[...]
    sin = jnp.sin(angle)
    first_run = lax.rem(lane, 32) < 16
    cos_tab[...] = jnp.cos(angle)
    sup_tab[...] = jnp.where(first_run, -sin, 0.0)
    sdn_tab[...] = jnp.where(first_run, 0.0, sin)

    loads["dl"].wait()
    loads["dr"].wait()
    normed = []
    low_l = low_r = None
    for d in range(tp):
        t = tpeer(d)
        if d:
            remote(mod_t.at[t], mod_t.at[t], mt_send.at[d], mt_recv.at[t], "tp", t).wait_recv()
        cols = pl.ds(pl.multiple_of(t * mcol, mcol), mcol)
        m = mod_t[t]
        nd = (base[:, cols] * (1.0 + m[1:2]) + m[0:1]).astype(BF16)
        normed.append((nd, cols))
        pl_, pr_ = dot(nd, dl[cols, :]), dot_t(nd, dr[:, cols])
        low_l = pl_ if low_l is None else low_l + pl_
        low_r = pr_ if low_r is None else low_r + pr_
    own = pl.ds(pl.multiple_of(me_t * rows, rows), rows)
    lat_buf[me_t, me_s, :rows, :] = rms(low_l, l_gain_ref[...]).astype(BF16)
    rk = turn(
        jnp.concatenate([low_r, low_r], axis=1), cos_tab[own, :], sup_tab[own, :], sdn_tab[own, :]
    )
    fold = lat_buf.shape[2] - rows
    fold_low = lax.broadcasted_iota(jnp.int32, (fold, 128), 1) < 64
    packed = [
        jnp.where(fold_low, rk[2 * j * fold:(2 * j + 1) * fold], rk[(2 * j + 1) * fold:(2 * j + 2) * fold])
        for j in range(rows // fold // 2)
    ]
    lat_buf[me_t, me_s, rows:, :] = jnp.concatenate(packed, axis=1).astype(BF16)
    mine = lat_buf.at[me_t, me_s]

    near = (lax.bitwise_xor(me_t, 1), lax.bitwise_xor(me_t, 2))
    far = lax.bitwise_xor(me_t, 3)

    def half(ref, k):
        cut = ref.shape[0] // 32 * 16
        return ref.at[pl.ds(0, cut)] if k == 0 else ref.at[pl.ds(cut, ref.shape[0] - cut)]

    def share(view, ssem, rsem, at):
        for k in range(2):
            c = remote(view, view, ssem.at[(*at, k)], rsem.at[(me_t, *at, 0)], "tp", near[k])
            c.start()
            sends.append(c)

    def relay(view, ssem, rsem, at, k):
        remote(view, view, ssem.at[(*at, k)], rsem.at[(near[k], *at, 0)], "tp", near[k]).wait_recv()
        piece = half(view, k)
        c = remote(piece, piece, ssem.at[(*at, 2 + k)], rsem.at[(near[k], *at, k)], "tp", near[1 - k])
        c.start()
        sends.append(c)

    def finish(view, ssem, rsem, at):
        for k in range(2):
            piece = half(view, k)
            remote(piece, piece, ssem.at[(*at, 2 + k)], rsem.at[(far, *at, k)], "tp", near[1 - k]).wait_recv()

    for d in range(1, sp):
        c = remote(mine, mine, lz_send.at[d], lz_recv.at[me_s], "sp", zpeer(d))
        c.start()
        sends.append(c)
    share(mine, lt_send, l_recv, (me_s,))
    loads["dq"].wait()
    low_q = None
    for nd, cols in normed:
        pq = dot(nd, dq[cols, :])
        low_q = pq if low_q is None else low_q + pq
    q_buf[me_t] = rms(low_q, q_gain_ref[...]).astype(BF16)
    share(q_buf.at[me_t], q_send, q_recv, ())

    def unfold(part):
        turned = []
        for j in range(part.shape[1] // 128):
            a = part[:, 128 * j:128 * (j + 1)].astype(F32)
            b = pltpu.roll(a, 64, 1)
            turned += [jnp.where(fold_low, a, b), jnp.where(fold_low, b, a)]
        return jnp.concatenate(turned, axis=0).astype(BF16)

    def expand(low, kr):
        kn = dot(low, uk[...]).astype(BF16)
        v = dot(low, uv[...]).astype(BF16)
        return (
            jnp.concatenate([kn[:, :QK_NOPE], kr], axis=1),
            jnp.concatenate([kn[:, QK_NOPE:], kr], axis=1),
            v,
        )

    for k in range(2):
        relay(lat_buf.at[near[k], me_s], lt_send, l_recv, (me_s,), k)
    for k in range(2):
        relay(q_buf.at[near[k]], q_send, q_recv, (), k)
    for d in range(1, sp):
        s = zpeer(d)
        slot = lat_buf.at[me_t, s]
        remote(slot, slot, lz_send.at[d], lz_recv.at[s], "sp", s).wait_recv()
        share(slot, lt_send, l_recv, (s,))

    loads["uk"].wait()
    loads["uv"].wait()
    for d in range(1, sp):
        s = zpeer(d)
        remote(ctx_buf.at[s], ctx_buf.at[s], cx_send.at[d], cx_recv.at[s], "sp", s).wait_recv()
    ctx_all = ctx_buf[...].reshape(-1, ctx_buf.shape[2])
    ctx_kv = expand(ctx_all[:, :kv_rank], ctx_all[:, kv_rank:])

    loads["uq"].wait()
    finish(q_buf.at[far], q_send, q_recv, ())
    q = dot(q_buf[...].reshape(group, q_buf.shape[2]), uq[...])
    one, two = q[:, 128:256], q[:, 256:384]
    low_half = lax.broadcasted_iota(jnp.int32, (group, 128), 1) < 64
    rope = turn(jnp.where(low_half, one, two), cos_tab[...], sup_tab[...], sdn_tab[...])
    nope = (q[:, :128], pltpu.roll(jnp.where(low_half, two, one), 64, 1))
    heads = (
        jnp.concatenate([nope[0], jnp.where(low_half, rope, 0.0)], axis=1).astype(BF16),
        jnp.concatenate([nope[1], jnp.where(low_half, 0.0, rope)], axis=1).astype(BF16),
    )
    factor = (QK_NOPE + QK_ROPE) ** (-0.5) * LOG2E

    def attend(state, kv, bias):
        result = []
        for h in range(2):
            s = dot_t(heads[h], kv[h]) * factor
            if bias:
                s = s + bias_ref[h] * LOG2E
            top = jnp.max(s, axis=-1, keepdims=True)
            v = kv[2][:, h * V_HEAD:(h + 1) * V_HEAD]
            if state is None:
                p = jnp.exp2(s - top)
                result.append((top, jnp.sum(p, axis=-1, keepdims=True), dot(p.astype(BF16), v)))
            else:
                m0, l0, a0 = state[h]
                top = jnp.maximum(top, m0)
                p = jnp.exp2(s - top)
                shrink = jnp.exp2(m0 - top)
                result.append((
                    top,
                    l0 * shrink + jnp.sum(p, axis=-1, keepdims=True),
                    a0 * shrink + dot(p.astype(BF16), v),
                ))
        return tuple(result)

    state = attend(None, ctx_kv, True)
    span = math.gcd(sp, 4)
    for d, t in enumerate((me_t, *near, far)):
        if d == 1:
            for e in range(1, sp):
                s = zpeer(e)
                for k in range(2):
                    relay(lat_buf.at[near[k], s], lt_send, l_recv, (s,), k)
        if d == 3:
            for e in range(sp):
                s = zpeer(e)
                finish(lat_buf.at[far, s], lt_send, l_recv, (s,))

        def chunk(i, st, t=t):
            block = lat_buf[t, pl.ds(i * span, span)]
            low = jnp.concatenate([block[j, :rows] for j in range(span)], axis=0)
            kr = jnp.concatenate([unfold(block[j, rows:]) for j in range(span)], axis=0)
            return attend(st, expand(low, kr), False)

        if sp == span:
            state = chunk(0, state)
        else:
            state = lax.fori_loop(0, sp // span, chunk, state)
    for h in range(2):
        att = (state[h][2] / state[h][1]).astype(BF16)
        att_src[:, :, h * V_HEAD:(h + 1) * V_HEAD] = att.reshape(tp, rows, V_HEAD)
    for d in range(1, tp):
        t = tpeer(d)
        c = remote(att_src.at[t], att_buf.at[me_t], a_send.at[d], a_recv.at[me_t], "tp", t)
        c.start()
        sends.append(c)
    loads["ow"].wait()
    width = att_src.shape[2]
    for d in range(tp):
        t = tpeer(d)
        if d == 0:
            block = att_src[me_t]
        else:
            remote(att_buf.at[t], att_buf.at[t], a_send.at[d], a_recv.at[t], "tp", t).wait_recv()
            block = att_buf[t]
        part = dot(block, ow[pl.ds(pl.multiple_of(t * width, width), width), :])
        if d == 0:
            mix[...] = part
        else:
            mix[...] += part
    for t in range(tp):
        cols = slice(t * mcol, (t + 1) * mcol)
        out_ref[:, cols] = (x_ref[:, cols].astype(F32) + mod_t[t][2:3] * mix[:, cols]).astype(BF16)
    for c in sends:
        c.wait_send()


def solution(mesh):
    sp, tp = mesh.shape["sp"], mesh.shape["tp"]

    def on_device(
        latent_in, condition, context_latent, context_rope, shift_weight, scale_weight,
        gate_weight, norm_gain, down_query, down_latent, down_rope, query_gain, latent_gain,
        up_query, up_key, up_value, context_bias, out_weight,
    ):
        rows, width = latent_in.shape
        n = QK_ROPE // 4
        inverse = np.tile(np.float32(ROPE_BASE) ** (-np.arange(n, dtype=np.float32) / n), 128 // n)
        inverse = inverse.astype(np.float32)[None]
        group = rows * tp
        any_ = pl.BlockSpec(memory_space=pl.ANY)
        vmem = pl.BlockSpec(memory_space=pltpu.VMEM)
        smem = pl.BlockSpec(memory_space=pltpu.SMEM)
        kv_rank, q_rank = down_latent.shape[1], down_query.shape[1]
        heads = up_key.shape[1] // QK_NOPE
        block = kv_rank + 2 * QK_ROPE
        dma = pltpu.SemaphoreType.DMA

        def like(a):
            return pltpu.VMEM(a.shape, a.dtype)

        return pl.pallas_call(
            functools.partial(kernel, sp, tp),
            out_shape=jax.ShapeDtypeStruct(latent_in.shape, latent_in.dtype),
            in_specs=[any_, vmem, any_, any_, any_, any_, any_, vmem, any_, any_, any_, vmem, vmem,
                      any_, any_, any_, smem, any_, vmem],
            out_specs=vmem,
            scratch_shapes=[
                like(latent_in), like(shift_weight), like(scale_weight), like(gate_weight),
                like(down_query), like(down_latent), like(down_rope.T), like(up_query), like(up_key),
                like(up_value), like(out_weight), like(context_rope.T),
                pltpu.VMEM((rows, width), F32),
                pltpu.VMEM((group, 128), F32), pltpu.VMEM((group, 128), F32),
                pltpu.VMEM((group, 128), F32),
                pltpu.VMEM((sp, 4, shift_weight.shape[1]), F32),
                pltpu.VMEM((tp, 4, shift_weight.shape[1]), F32),
                pltpu.VMEM((sp, context_latent.shape[0], block), BF16),
                pltpu.VMEM((tp, sp, rows + rows * QK_ROPE // kv_rank, kv_rank), BF16),
                pltpu.VMEM((tp, rows, q_rank), BF16),
                pltpu.VMEM((tp, rows, heads * V_HEAD), BF16),
                pltpu.VMEM((tp, rows, heads * V_HEAD), BF16),
                pltpu.VMEM((rows, width), F32),
                dma((13,)),
                dma((sp,)), dma((sp,)), dma((tp,)), dma((tp,)), dma((sp,)), dma((sp,)),
                dma((sp,)), dma((sp,)), dma((sp, 4)), dma((tp, sp, 2)),
                dma((4,)), dma((tp, 2)), dma((tp,)), dma((tp,)),
            ],
            compiler_params=pltpu.CompilerParams(
                collective_id=0, has_side_effects=True, vmem_limit_bytes=60 * 1024 * 1024
            ),
        )(
            latent_in, condition[None], context_latent, context_rope.T, shift_weight, scale_weight,
            gate_weight, norm_gain[None], down_query, down_latent, down_rope.T, query_gain[None],
            latent_gain[None], up_query, up_key, up_value, context_bias, out_weight, inverse,
        )

    in_specs = (
        P(("dp", "sp", "tp"), None), P(("dp", "sp")), P(("dp", "sp"), None), P(("dp", "sp"), None),
        P("sp", "tp"), P("sp", "tp"), P("sp", "tp"), P(), P(), P(), P(), P(), P(),
        P(None, "tp"), P(None, "tp"), P(None, "tp"), P("tp"), P(),
    )
    return jax.shard_map(
        on_device, mesh=mesh, in_specs=in_specs, out_specs=P(("dp", "sp", "tp"), None), check_vma=False
    )
```
